32 devices in a mesh: rep: 2 (over x), fs: 8 (over z, y), tp: 2 (over core).
Axes of the slice: x: 2, y: 2, z: 4, core: 2. Of those that a mesh axis runs over, the one named last changes fastest.
Arguments:
- inputs: bfloat16 [8192, 2048], P(('rep', 'fs')), may hold values from -6 to 6
- cotangent: bfloat16 [8192, 2048], P(('rep', 'fs')), may hold values from -6 to 6
- gate_weight: bfloat16 [2048, 4096], P('fs', 'tp'), may hold values from -0.125 to 0.125
- up_weight: bfloat16 [2048, 4096], P('fs', 'tp'), may hold values from -0.125 to 0.125
- down_weight: bfloat16 [2048, 4096], P('fs', 'tp'), may hold values from -0.09375 to 0.09375
Outputs:
- grad_input: bfloat16 [8192, 2048], P(('rep', 'fs'))
- grad_down: float32 [2048, 4096], P('fs', 'tp')
The draws below stay inside these ranges and needn't reach their ends.
All inputs are finite; a program needn't handle non-finite values.
Results may differ from the reference program's by a relative error of at most 0.014.
Values may be sent and summed in bfloat16 or wider, within the bound.
No kernel may reach another device: no remote copies, remote signals or barrier semaphores. Data moves between devices by JAX's collectives and lax.ppermute only.
A program may use at most 128 MiB of HBM per device.

```python
import jax
import jax.numpy as jnp
from jax import lax

D = 2048
FF = 4096
TOK_DEV = 512
TOKENS = 8192
N_TP = 2


def raised(values, key, source, target, shards_of, factor):
    owner, partner = [(jnp.arange(values.shape[axis_at]) // (values.shape[axis_at] // shards_of)).reshape([-1 if axis == axis_at else 1 for axis in range(values.ndim)]) for axis_at in (source, target)]
    chosen = jax.random.permutation(key, shards_of)[partner]
    strong = (owner == chosen) | (owner == (partner + shards_of // 2) % shards_of)
    return jnp.where(strong, factor * values, values)


def shard_levels(stream_key, shape, cuts, low, high):
    loudness, own = 1.0, jax.random.fold_in(stream_key, 6)
    for position, shards_of in cuts:
        draws = jnp.exp(jax.random.uniform(jax.random.fold_in(own, position), (shards_of,), jnp.float32, low / len(cuts), high / len(cuts)))
        loudness = loudness * jnp.repeat(draws, shape[position] // shards_of).reshape([-1 if axis == position else 1 for axis in range(len(shape))])
    return loudness


def normal_values(stream_key, dims, scale, most, split=(), held_as=jnp.bfloat16):
    entries = scale * jax.random.normal(stream_key, dims, jnp.float32)
    if split:
        entries = entries * shard_levels(stream_key, dims, split, -0.22, 0.18)
    return jnp.clip(entries, -most, most).astype(held_as)


def heavy_noise(rng, extent, width, most, cuts, heavy, kind=jnp.bfloat16):
    result = width * jax.random.normal(rng, extent, jnp.float32)
    if cuts:
        result = result * shard_levels(rng, extent, cuts, -0.22, 0.18)
    return jnp.clip(raised(result, jax.random.fold_in(rng, 3), *heavy), -most, most).astype(kind)


def setup_inputs(seed: int = 0) -> dict:
    splits = jax.random.split(jax.random.key(seed), 6)
    inputs = normal_values(splits[0], (TOKENS, D), 1.0, 6.0, ((0, 16),))
    cotangent = heavy_noise(splits[1], (TOKENS, D), 1.0, 6.0, ((0, 16),), (0, 1, 16, 2.0))
    gate_weight = normal_values(splits[2], (D, FF), D ** -0.5, 0.125, ((0, 8), (1, 2)))
    up_weight = normal_values(splits[3], (D, FF), D ** -0.5, 0.125, ((0, 8), (1, 2)))
    down_weight = normal_values(splits[4], (D, FF), FF ** -0.5, 0.09375, ((0, 8), (1, 2)))
    return dict(inputs=inputs, cotangent=cotangent, gate_weight=gate_weight, up_weight=up_weight, down_weight=down_weight)


def reference(inputs, cotangent, gate_weight, up_weight, down_weight):
    hid_width = FF // N_TP
    contract = (((1,), (1,)), ((), ()))
    contract_tok = (((0,), (0,)), ((), ()))

    def one_block(grad_acc, block_index):
        row_start = (block_index * TOK_DEV).astype(jnp.int32)
        in_rows = lax.dynamic_slice_in_dim(inputs, row_start, TOK_DEV, 0)
        cot_rows = lax.dynamic_slice_in_dim(cotangent, row_start, TOK_DEV, 0)
        gate_val = jnp.dot(in_rows, gate_weight, preferred_element_type=jnp.float32)
        up_val = jnp.dot(in_rows, up_weight, preferred_element_type=jnp.float32)
        sigmoid_gate = jax.nn.sigmoid(gate_val)
        active = gate_val * sigmoid_gate
        hidden = (active * up_val).astype(jnp.bfloat16)
        grad_hidden = jnp.dot(cot_rows, down_weight, preferred_element_type=jnp.float32)
        grad_gate = (grad_hidden * up_val * sigmoid_gate * (1.0 + gate_val * (1.0 - sigmoid_gate))).astype(jnp.bfloat16)
        grad_up = (grad_hidden * active).astype(jnp.bfloat16)
        total = jnp.zeros((TOK_DEV, D), jnp.float32)
        for blk in range(N_TP):
            lo_col = blk * hid_width
            hi_col = lo_col + hid_width
            piece = lax.dot_general(grad_gate[:, lo_col:hi_col], gate_weight[:, lo_col:hi_col], contract, preferred_element_type=jnp.float32)
            piece = piece + lax.dot_general(grad_up[:, lo_col:hi_col], up_weight[:, lo_col:hi_col], contract, preferred_element_type=jnp.float32)
            rounded = lax.optimization_barrier(piece.astype(jnp.bfloat16))
            total = total + rounded.astype(jnp.float32)
        grad_acc = grad_acc + lax.dot_general(cot_rows, hidden, contract_tok, preferred_element_type=jnp.float32)
        return grad_acc, total.astype(jnp.bfloat16)

    indices = jnp.arange(TOKENS // TOK_DEV, dtype=jnp.int32)
    grad_acc, pieces = lax.scan(one_block, jnp.zeros((D, FF), jnp.float32), indices)
    grad_input = pieces.reshape(TOKENS, D)
    grad_down = grad_acc * (float(TOKENS) ** -0.5)
    return grad_input, grad_down
```

```python
import math

import jax
import jax.numpy as jnp
from jax import lax
from jax.sharding import PartitionSpec as P


F32, BF16 = jnp.float32, jnp.bfloat16
ROWS_BY_ROWS = (((0,), (0,)), ((), ()))
COLS_BY_COLS = (((1,), (1,)), ((), ()))


def on_device(sizes, inputs, cotangent, gate_weight, up_weight, down_weight):
    n_rep, n_fs, n_tp = sizes["rep"], sizes["fs"], sizes["tp"]
    n_ring = n_fs // 2
    x = lax.axis_index("rep")
    f = lax.axis_index("fs")
    c = lax.axis_index("tp")
    g, p = f // 2, f % 2
    tok, width = inputs.shape
    unit = width // n_ring
    cols = gate_weight.shape[1]
    half, quarter = cols // 2, cols // (2 * n_rep)
    part = tok // n_tp

    pair = [(i, i ^ 1) for i in range(n_fs)]

    def ring(shift):
        return [(i, (i // 2 + shift) % n_ring * 2 + i % 2) for i in range(n_fs)]

    def turn(n, shift):
        return [(i, (i + shift) % n) for i in range(n)]

    def over_pair(v):
        return lax.ppermute(v, "fs", pair)

    def over_ring(v, shift):
        return lax.ppermute(v, "fs", ring(shift))

    def from_rep(v, k):
        return lax.ppermute(v, "rep", turn(n_rep, -k))

    def from_tp(v, k):
        return lax.ppermute(v, "tp", turn(n_tp, -k))

    def col_slice(v, start, size):
        return lax.dynamic_slice(v, (0, start), (v.shape[0], size))

    def row_slice(v, start, size):
        return lax.dynamic_slice(v, (start, 0), (size, v.shape[1]))

    def to_ring(v):
        return jnp.concatenate([col_slice(v, (g - s) % n_ring * unit, unit) for s in range(n_ring)], axis=1)

    def gathered(weight):
        mine = col_slice(weight, p * half, half)
        other = over_pair(col_slice(weight, (1 - p) * half, half))
        both = jnp.where(p == 0, jnp.concatenate([mine, other], 0), jnp.concatenate([other, mine], 0))
        own = [col_slice(both, (x + k) % n_rep * quarter, quarter) for k in range(n_rep)]
        blocks = [None] * n_ring
        blocks[0] = own[0]
        for s in range(1, n_ring // 2 + 1):
            blocks[s] = over_ring(blocks[s - 1], 1)
            t = n_ring - s
            if t > n_ring // 2:
                blocks[t] = over_ring(blocks[(t + 1) % n_ring], -1)
        full = [jnp.concatenate(blocks, 0)]
        for k in range(1, n_rep):
            full.append(jnp.concatenate([own[k]] + [from_rep(b, k) for b in blocks[1:]], 0))
        return full

    def all_tokens(v):
        v = to_ring(v)
        theirs = over_pair(row_slice(v, c * part, part))
        return jnp.concatenate([v, theirs] + [from_tp(theirs, k) for k in range(1, n_tp)], 0)

    gate_w = gathered(gate_weight)
    up_w = gathered(up_weight)
    toks = all_tokens(inputs)
    down_w = gathered(down_weight)
    cots = all_tokens(cotangent)

    def dots(a, ws):
        return [jnp.dot(a, w, preferred_element_type=F32) for w in ws]

    gate_val, up_val = dots(toks, gate_w), dots(toks, up_w)
    sig = [jax.nn.sigmoid(v) for v in gate_val]
    active = [v * s for v, s in zip(gate_val, sig)]
    hidden = [(a * u).astype(BF16) for a, u in zip(active, up_val)]

    grads = [lax.dot_general(cots, h, ROWS_BY_ROWS, preferred_element_type=F32) for h in hidden]
    order = list(range(n_ring // 2, 0, -1)) + list(range(n_ring // 2 + 1, n_ring)) + [0]
    summed = {}
    for s in order:
        rows = slice(s * unit, (s + 1) * unit)
        total = grads[0][rows]
        for k in range(1, n_rep):
            total = total + from_rep(grads[n_rep - k][rows].astype(BF16), k).astype(F32)
        summed[s] = total
    carry = summed[n_ring // 2]
    for s in range(n_ring // 2, 0, -1):
        got = over_ring(carry.astype(BF16), -1).astype(F32)
        carry = summed[s - 1] + got
    back = None
    for s in range(n_ring // 2 + 1, n_ring):
        back = summed[s] if back is None else summed[s] + back
        back = over_ring(back.astype(BF16), 1).astype(F32)
    shard = carry if back is None else carry + back
    shard = shard.astype(BF16)
    keep = row_slice(shard, p * (unit // 2), unit // 2)
    give = row_slice(shard, (1 - p) * (unit // 2), unit // 2)
    pieces = {}
    for k in range(n_rep):
        if k == 0:
            pieces[0, 0], pieces[1, 0] = keep, over_pair(give)
        else:
            pieces[0, k] = from_rep(keep, k)
            diagonal = [
                (i * n_fs + j, (i - k) % n_rep * n_fs + (j ^ 1))
                for i in range(n_rep)
                for j in range(n_fs)
            ]
            pieces[1, k] = lax.ppermute(give, ("rep", "fs"), diagonal)
    stacked = jnp.stack([pieces[d, k] for d in range(2) for k in range(n_rep)])
    scale = 1.0 / math.sqrt(tok * n_fs * n_rep)
    grad_down = jnp.concatenate(
        [
            lax.dynamic_index_in_dim(stacked, (h + p) % 2 * n_rep + (q - x) % n_rep, 0, False)
            for h in range(2)
            for q in range(n_rep)
        ],
        axis=1,
    ).astype(F32) * scale

    grad_hidden = dots(cots, down_w)
    grad_gate = [
        (gh * u * s * (1.0 + v * (1.0 - s))).astype(BF16)
        for gh, u, s, v in zip(grad_hidden, up_val, sig, gate_val)
    ]
    grad_up = [(gh * a).astype(BF16) for gh, a in zip(grad_hidden, active)]

    def back_through(rows):
        total = 0.0
        for gs, ws in ((grad_gate, gate_w), (grad_up, up_w)):
            for gr, w in zip(gs, ws):
                total = total + lax.dot_general(gr[rows], w, COLS_BY_COLS, preferred_element_type=F32)
        return total.astype(BF16)

    theirs = back_through(slice(tok, 2 * tok))
    total = theirs[:part].astype(F32)
    for k in range(1, n_tp):
        total = total + from_tp(theirs[(n_tp - k) * part : (n_tp - k + 1) * part], k).astype(F32)
    arrived = over_pair(total.astype(BF16))
    ours = back_through(slice(0, tok))
    own_total = ours.astype(F32)
    for k in range(1, n_tp):
        own_total = own_total + from_tp(ours, k).astype(F32)
    rel = jnp.stack([arrived] + [from_tp(arrived, k) for k in range(1, n_tp)])
    arrived_all = jnp.concatenate(
        [lax.dynamic_index_in_dim(rel, (i - c) % n_tp, 0, False) for i in range(n_tp)], 0
    )
    summed_in = (own_total + arrived_all.astype(F32)).astype(BF16)
    grad_input = jnp.concatenate(
        [col_slice(summed_in, (g - b) % n_ring * unit, unit) for b in range(n_ring)], axis=1
    )
    return grad_input, grad_down


def solution(mesh):
    placed = (
        P(("rep", "fs"), None),
        P(("rep", "fs"), None),
        P("fs", "tp"),
        P("fs", "tp"),
        P("fs", "tp"),
    )
    sizes = dict(mesh.shape)

    def body(*args):
        return on_device(sizes, *args)

    return jax.shard_map(
        body,
        mesh=mesh,
        in_specs=placed,
        out_specs=(P(("rep", "fs"), None), P("fs", "tp")),
        check_vma=False,
    )
```
